32 devices in a mesh: rep: 2 (over x), fs: 8 (over z, y), tp: 2 (over core).
Axes of the slice: x: 2, y: 2, z: 4, core: 2. Of those that a mesh axis runs over, the one named last changes fastest.
Arguments:
- hidden_in: bfloat16 [10240, 2048], P(('rep', 'fs'), 'tp'), may hold values from -6 to 6
- mix_gain: float32 [2048], replicated, may hold values from 0.1 to 1.9
- w_value: bfloat16 [2048, 1024], P('fs', 'tp'), may hold values from -0.125 to 0.125
- w_gate: bfloat16 [2048, 1024], P('fs', 'tp'), may hold values from -0.125 to 0.125
- conv_taps: float32 [31, 1024], P(None, 'tp'), may hold values from -5 to 5
- conv_bias: float32 [1024], P('tp'), may hold values from -3 to 3
- chan_gain: float32 [1024], P('tp'), may hold values from 0.1 to 1.9
- chan_bias: float32 [1024], P('tp'), may hold values from -3 to 3
- w_back: bfloat16 [1024, 2048], P('tp', 'fs'), may hold values from -0.1875 to 0.1875
- feed_gain: float32 [2048], replicated, may hold values from 0.1 to 1.9
- w_up: bfloat16 [2048, 8192], P(None, ('fs', 'tp')), may hold values from -0.125 to 0.125
- w_down: bfloat16 [8192, 2048], P(('fs', 'tp')), may hold values from -0.0625 to 0.0625
Outputs:
- layer_out: bfloat16 [10240, 2048], P(('rep', 'fs'), 'tp')
The draws below stay inside these ranges and needn't reach their ends.
All inputs are finite; a program needn't handle non-finite values.
Results may differ from the reference program's by a relative error of at most 0.015.
Values may be sent and summed in bfloat16 or wider, within the bound.
No kernel may reach another device: no remote copies, remote signals or barrier semaphores. Data moves between devices by JAX's collectives and lax.ppermute only.
A program may use at most 128 MiB of HBM per device.

```python
import jax
import jax.numpy as jnp
from jax import lax

D = 2048
CH = 1024
FF = 8192
KW = 31
LEN = 128
TOKENS = 10240
N_FS = 8
N_TP = 2


def draw_conv_taps(key, part):
    entry_key, rough_key = jax.random.split(jax.random.fold_in(key, 11))
    channel_ramp = jnp.arange(CH, dtype=jnp.float32) / CH
    roughness = jax.random.uniform(rough_key, (KW, CH), jnp.float32, 0.5, 1.5)
    entries = jnp.clip(jax.random.normal(entry_key, (KW, CH), jnp.float32), -4.0, 4.0)
    growth = 3.0 ** channel_ramp
    return (entries * roughness * growth[None, :] * KW ** (-0.5)).astype(jnp.float32)


def shard_levels(own_key, dims, cuts, least, high):
    loudness, own = 1.0, jax.random.fold_in(own_key, 6)
    for dim, blocks in cuts:
        heights = jnp.exp(jax.random.uniform(jax.random.fold_in(own, dim), (blocks,), jnp.float32, least / len(cuts), high / len(cuts)))
        loudness = loudness * jnp.repeat(heights, dims[dim] // blocks).reshape([-1 if axis == dim else 1 for axis in range(len(dims))])
    return loudness


def gaussian(own_key, extent, deviation, most, cuts=(), kind=jnp.bfloat16):
    values = deviation * jax.random.normal(own_key, extent, jnp.float32)
    if cuts:
        values = values * shard_levels(own_key, extent, cuts, -0.22, 0.18)
    return jnp.clip(values, -most, most).astype(kind)


def setup_inputs(seed: int = 0) -> dict:
    key_of = jax.random.split(jax.random.key(seed), 13)
    hidden_in = gaussian(key_of[0], (TOKENS, D), 1.0, 6.0, ((0, 16), (1, 2)))
    mix_gain = jnp.clip(1.0 + 0.18 * jax.random.normal(key_of[1], (D,), jnp.float32), 0.1, 1.9)
    w_value = gaussian(key_of[2], (D, CH), D ** -0.5, 0.125, ((0, 8), (1, 2)))
    w_gate = gaussian(key_of[3], (D, CH), D ** -0.5, 0.125, ((0, 8), (1, 2)))
    conv_taps = draw_conv_taps(jax.random.fold_in(key_of[12], 71), 0)
    conv_bias = gaussian(key_of[5], (CH,), 0.5, 3.0, ((0, 2),), jnp.float32)
    chan_gain = jnp.clip(1.0 + 0.18 * jax.random.normal(key_of[6], (CH,), jnp.float32), 0.1, 1.9)
    chan_bias = gaussian(key_of[7], (CH,), 0.5, 3.0, ((0, 2),), jnp.float32)
    w_back = gaussian(key_of[8], (CH, D), CH ** -0.5, 0.1875, ((0, 2), (1, 8)))
    feed_gain = jnp.clip(1.0 + 0.18 * jax.random.normal(key_of[9], (D,), jnp.float32), 0.1, 1.9)
    w_up = gaussian(key_of[10], (D, FF), D ** -0.5, 0.125, ((1, 16),))
    w_down = gaussian(key_of[11], (FF, D), FF ** -0.5, 0.0625, ((0, 16),))
    return dict(hidden_in=hidden_in, mix_gain=mix_gain, w_value=w_value, w_gate=w_gate, conv_taps=conv_taps, conv_bias=conv_bias, chan_gain=chan_gain, chan_bias=chan_bias, w_back=w_back, feed_gain=feed_gain, w_up=w_up, w_down=w_down)


def rms_norm(stream, gain):
    values = stream.astype(jnp.float32)
    scaled = values * lax.rsqrt(lax.optimization_barrier(jnp.mean(values * values, axis=-1, keepdims=True)) + 1e-06)
    return (scaled * gain).astype(jnp.bfloat16)

def causal_filter(gated, conv_taps, conv_bias):
    channels = gated.shape[1]
    blocks = gated.reshape(gated.shape[0] // LEN, LEN, channels)
    padded = jnp.pad(blocks, ((0, 0), (KW - 1, 0), (0, 0)))
    result = jnp.zeros_like(blocks) + conv_bias
    for tap_index in range(KW):
        result = result + conv_taps[tap_index] * padded[:, tap_index:tap_index + LEN]
    return result.reshape(gated.shape)

def blocked_sum(left, right):
    inner = left.shape[1] // N_TP
    running = jnp.zeros((left.shape[0], right.shape[1]), jnp.float32)
    for block_index in range(N_TP):
        partial_value = jnp.dot(left[:, block_index * inner:(block_index + 1) * inner], right[block_index * inner:(block_index + 1) * inner], preferred_element_type=jnp.float32)
        running = running + partial_value.astype(jnp.bfloat16).astype(jnp.float32)
    return running

def strided_sum(left, right):
    rows = left.shape[0]
    width = right.shape[1]
    block = left.shape[1] // (N_FS * N_TP)
    left_blocks = left.reshape(rows, N_FS, N_TP, block)
    right_blocks = right.reshape(N_FS, N_TP, block, width)
    running = jnp.zeros((rows, width), jnp.float32)
    for block_index in range(N_TP):
        partial_value = jnp.dot(left_blocks[:, :, block_index].reshape(rows, N_FS * block), right_blocks[:, block_index].reshape(N_FS * block, width), preferred_element_type=jnp.float32)
        running = running + partial_value.astype(jnp.bfloat16).astype(jnp.float32)
    return running

def reference(hidden_in, mix_gain, w_value, w_gate, conv_taps, conv_bias, chan_gain, chan_bias, w_back, feed_gain, w_up, w_down):
    normed = rms_norm(hidden_in, mix_gain)
    value_proj = jnp.dot(normed, w_value, preferred_element_type=jnp.float32)
    gate_proj = jnp.dot(normed, w_gate, preferred_element_type=jnp.float32)
    gated = value_proj * jax.nn.sigmoid(gate_proj)
    filtered = causal_filter(gated, conv_taps, conv_bias)
    chan_mean = lax.optimization_barrier(jnp.mean(filtered, axis=1, keepdims=True))
    chan_var = lax.optimization_barrier(jnp.mean(filtered * filtered, axis=1, keepdims=True)) - chan_mean * chan_mean
    centred = (filtered - chan_mean) * lax.rsqrt(chan_var + 1e-05) * chan_gain + chan_bias
    mixer_act = jax.nn.silu(centred).astype(jnp.bfloat16)
    mixed = blocked_sum(mixer_act, w_back)
    second = (hidden_in.astype(jnp.float32) + mixed).astype(jnp.bfloat16)
    normed_feed = rms_norm(second, feed_gain)
    up_proj = jnp.dot(normed_feed, w_up, preferred_element_type=jnp.float32)
    hidden = jnp.square(jax.nn.relu(up_proj)).astype(jnp.bfloat16)
    feed = strided_sum(hidden, w_down)
    return (second.astype(jnp.float32) + feed).astype(jnp.bfloat16)
```

```python
import jax
import jax.numpy as jnp
from jax import lax
from jax.sharding import PartitionSpec as P


LEN = 128
BF = jnp.bfloat16
F32 = jnp.float32


def rms_norm(stream, gain):
    values = stream.astype(F32)
    scaled = values * lax.rsqrt(jnp.mean(values * values, axis=-1, keepdims=True) + 1e-06)
    return (scaled * gain).astype(BF)


def causal_filter(gated, conv_taps, conv_bias):
    taps, channels = conv_taps.shape
    blocks = gated.reshape(gated.shape[0] // LEN, LEN, channels)
    padded = jnp.pad(blocks, ((0, 0), (taps - 1, 0), (0, 0)))
    result = jnp.zeros_like(blocks) + conv_bias
    for tap_index in range(taps):
        result = result + conv_taps[tap_index] * padded[:, tap_index : tap_index + LEN]
    return result.reshape(gated.shape)


def half(array, axis, index):
    size = array.shape[axis] // 2
    return lax.dynamic_slice_in_dim(array, index * size, size, axis)


def flip(array, axis, bit):
    n = lax.axis_size(axis)
    return lax.ppermute(array, axis, [(i, i ^ bit) for i in range(n)])


def gather_shards(shard, axis, side):
    n = lax.axis_size("fs")
    got = {0: half(shard, axis, side)}
    bit = n // 2
    while bit > 1:
        for j in list(got):
            got[j | bit] = flip(got[j], "fs", bit)
        bit //= 2
    pieces = [(0, None, shard), (1, None, flip(shard, "fs", 1))]
    for j in sorted(got):
        if j:
            got[j | 1] = flip(got[j], "fs", 1)
    for j in sorted(got):
        if j > 1:
            pieces.append((j, 0, got[j]))
            pieces.append((j, 1, flip(got[j], "rep", 1)))
    return pieces


def assemble(pieces, axis, place, side):
    size = pieces[0][2].shape[axis]
    shape = list(pieces[0][2].shape)
    shape[axis] = size * lax.axis_size("fs")
    whole = jnp.zeros(shape, BF)
    for j, part, piece in pieces:
        start = (place ^ j) * size
        if part is not None:
            start = start + (side if part == 0 else 1 - side) * (size // 2)
        whole = lax.dynamic_update_slice_in_dim(whole, piece, start, axis)
    return whole


def other_weights(shard, axis, side):
    n = lax.axis_size("fs")
    mine = half(shard, axis, side)
    parts = []
    for bit in range(4, n, 4):
        near = flip(mine, "fs", bit)
        far = flip(near, "rep", 1)
        parts += [near, far]
    parts += [flip(p, "tp", 1) for p in parts]
    return jnp.concatenate(parts, axis)


def feed(rows, up, down):
    hidden = jnp.square(jax.nn.relu(jnp.dot(rows, up, preferred_element_type=F32))).astype(BF)
    return jnp.dot(hidden, down, preferred_element_type=F32)


def shards(
    hidden_in,
    mix_gain,
    w_value,
    w_gate,
    conv_taps,
    conv_bias,
    chan_gain,
    chan_bias,
    w_back,
    feed_gain,
    w_up,
    w_down,
):
    place, side, core = lax.axis_index("fs"), lax.axis_index("rep"), lax.axis_index("tp")
    rows = hidden_in.shape[0]
    own = rows // 2
    width = hidden_in.shape[1]
    channels = w_value.shape[1]

    peer_in = flip(hidden_in, "tp", 1)
    gathered = jnp.where(
        core == 0,
        jnp.concatenate([hidden_in, peer_in], 1),
        jnp.concatenate([peer_in, hidden_in], 1),
    )
    gate_pieces = gather_shards(jnp.concatenate([w_value, w_gate], 1), 0, side)
    back_pieces = gather_shards(w_back, 1, side)
    normed = rms_norm(gathered, mix_gain)
    both = jnp.dot(normed, assemble(gate_pieces, 0, place, side), preferred_element_type=F32)
    gated = both[:, :channels] * jax.nn.sigmoid(both[:, channels:])
    filtered = causal_filter(gated, conv_taps, conv_bias)
    stats = jnp.stack([jnp.sum(filtered, axis=1), jnp.sum(filtered * filtered, axis=1)])
    stats = (stats + flip(stats, "tp", 1)) / (2 * channels)
    chan_mean = stats[0][:, None]
    chan_var = stats[1][:, None] - chan_mean * chan_mean
    centred = (filtered - chan_mean) * lax.rsqrt(chan_var + 1e-05) * chan_gain + chan_bias
    mixer_act = jax.nn.silu(centred).astype(BF)
    partial = jnp.dot(
        mixer_act, assemble(back_pieces, 1, place, side), preferred_element_type=F32
    ).astype(BF)
    mixed = half(partial, 0, core).astype(F32) + flip(half(partial, 0, 1 - core), "tp", 1).astype(F32)
    second = (half(gathered, 0, core).astype(F32) + mixed).astype(BF)
    normed_feed = rms_norm(second, feed_gain)

    up_own = jnp.concatenate([w_up, flip(w_up, "tp", 1)], 1)
    down_own = jnp.concatenate([w_down, flip(w_down, "tp", 1)], 0)
    up_far = other_weights(w_up, 1, side)
    down_far = other_weights(w_down, 0, side)

    q = own // 2
    a0, b0 = normed_feed[:q], normed_feed[q:]
    a2, b1 = flip(a0, "fs", 2), flip(b0, "fs", 1)
    a1, b2 = flip(a0, "fs", 1), flip(b0, "fs", 2)
    a3, b3 = flip(a2, "fs", 1), flip(b1, "fs", 2)
    out = []
    for blocks, first, then in (((a0, a1, a2, a3), 1, 2), ((b0, b1, b2, b3), 2, 1)):
        tokens = jnp.concatenate(blocks, 0)
        sums = (feed(tokens, up_own, down_own) + feed(tokens, up_far, down_far)).astype(BF)
        o = [sums[j * q : (j + 1) * q] for j in range(4)]
        got_far = flip(o[3], "fs", first)
        got_near = flip(o[first], "fs", first)
        passed = (o[then].astype(F32) + got_far.astype(F32)).astype(BF)
        last = flip(passed, "fs", then)
        out.append(o[0].astype(F32) + got_near.astype(F32) + last.astype(F32))
    layer = (second.astype(F32) + jnp.concatenate(out, 0)).astype(BF)
    keep, give = half(layer, 1, core), half(layer, 1, 1 - core)
    took = flip(give, "tp", 1)
    return jnp.where(
        core == 0, jnp.concatenate([keep, took], 0), jnp.concatenate([took, keep], 0)
    )


def solution(mesh):
    placed = (
        P(("rep", "fs"), "tp"),
        P(),
        P("fs", "tp"),
        P("fs", "tp"),
        P(None, "tp"),
        P("tp"),
        P("tp"),
        P("tp"),
        P("tp", "fs"),
        P(),
        P(None, ("fs", "tp")),
        P(("fs", "tp"), None),
    )
    return jax.shard_map(
        shards, mesh=mesh, in_specs=placed, out_specs=P(("rep", "fs"), "tp"), check_vma=False
    )
```
